256 devices in a mesh: ep: 64 (over z, x, core), tp: 4 (over y).
Axes of the slice: x: 4, y: 4, z: 8, core: 2. Of those that a mesh axis runs over, the one named last changes fastest.
Arguments:
- mixer_input: bfloat16 [40960, 2048], P('ep'), may hold values from -6 to 6
- mixer_gain: float32 [2048], replicated, may hold values from 0.1 to 1.9
- value_weight: bfloat16 [2048, 1024], P(None, 'tp'), may hold values from -0.125 to 0.125
- inner_gate: bfloat16 [2048, 1024], P(None, 'tp'), may hold values from -0.125 to 0.125
- outer_gate: bfloat16 [2048, 1024], P(None, 'tp'), may hold values from -0.125 to 0.125
- kernel_taps: float32 [3, 1024], P(None, 'tp'), may hold values from -3 to 3
- mixer_proj: bfloat16 [1024, 2048], P('tp'), may hold values from -0.1875 to 0.1875
- expert_input: bfloat16 [40960, 2048], P(('ep', 'tp')), may hold values from -6 to 6
- expert_gain: float32 [2048], replicated, may hold values from 0.1 to 1.9
- routes: int32 [40960, 2], P(('ep', 'tp')), may hold values from 0 to 63, as said below
- group_logits: float32 [40960, 8], P(('ep', 'tp')), may hold values from -6 to 6
- pair_logits: float32 [40960, 2], P(('ep', 'tp')), may hold values from -6 to 6
- gate_weight: bfloat16 [64, 2048, 1024], P('ep', None, 'tp'), may hold values from -0.125 to 0.125
- up_weight: bfloat16 [64, 2048, 1024], P('ep', None, 'tp'), may hold values from -0.125 to 0.125
- down_weight: bfloat16 [64, 1024, 2048], P('ep', 'tp'), may hold values from -0.75 to 0.75
Outputs:
- mixer_output: bfloat16 [40960, 2048], P(('ep', 'tp'))
- expert_output: bfloat16 [40960, 2048], P(('ep', 'tp'))
The draws below stay inside these ranges and needn't reach their ends.
Inputs may be any that keep to these rules, and one draw needn't show every extreme that they name: `routes`: both entries of a row are different experts of one group (equal after integer division by 8). In the rows of one device every group is chosen by the same number of rows, no expert is named more than 10 times, and in every draw one expert is named exactly 10 times in the rows of every device.
All inputs are finite; a program needn't handle non-finite values.
Results may differ from the reference program's by a relative error of at most 0.01.
Values may be sent and summed in bfloat16 or wider, within the bound.
A program may use at most 128 MiB of HBM per device.

```python
import jax
import jax.numpy as jnp
from jax import lax

D = 2048
CW = 1024
TAPS = 3
FF = 1024
EPG = 8
TOK_DEV = 160
GROUPS = 8
EXPERTS = 64
CAP = 10
TOKENS = 40960
N_EP = 64
N_TP = 4


def route_block(key, heavy, light):
    share = CAP // 2
    keys = jax.random.split(key, 4)
    group = jax.random.randint(keys[0], (), 0, GROUPS)
    order = jax.random.permutation(keys[1], EPG)
    raised = group * EPG + order[0]
    lowered = group * EPG + order[1]
    if share >= 2:
        shift = jax.random.randint(keys[2], (), 1, share)
    else:
        shift = jnp.zeros((), jnp.int32)
    clear = (raised != heavy) & (raised != light) & (lowered != heavy) & (lowered != light)
    shift = jnp.where(clear, shift, 0)
    experts_iota = jnp.arange(EXPERTS, dtype=jnp.int32)
    loads = (share + share * (experts_iota == heavy) - share * (experts_iota == light) + shift * (experts_iota == raised) - shift * (experts_iota == lowered)).astype(jnp.int32)
    bounds = jnp.cumsum(loads)
    per_group = EPG * share // 2
    place = jnp.arange(TOK_DEV, dtype=jnp.int32)
    first_slot = place // per_group * (2 * per_group) + place % per_group
    second_slot = first_slot + per_group
    first = jnp.sum((bounds[None, :] <= first_slot[:, None]).astype(jnp.int32), axis=1)
    second = jnp.sum((bounds[None, :] <= second_slot[:, None]).astype(jnp.int32), axis=1)
    pairs = jnp.stack([first, second], axis=1).astype(jnp.int32)
    shuffle = jax.random.permutation(keys[3], TOK_DEV)
    return jnp.zeros((TOK_DEV, 2), jnp.int32).at[shuffle].set(pairs)


def draw_routes(key, part):
    base = jax.random.fold_in(key, 17)
    picks = jax.random.split(jax.random.fold_in(base, 1), 2)
    group = jax.random.randint(picks[0], (), 0, GROUPS)
    order = jax.random.permutation(picks[1], EPG)
    heavy = group * EPG + order[0]
    light = group * EPG + order[1]
    block_keys = jax.random.split(jax.random.fold_in(base, 2), TOKENS // TOK_DEV)

    def one_block(block_key):
        return route_block(block_key, heavy, light)
    routed = jax.vmap(one_block)(block_keys)
    return routed.reshape(TOKENS, 2)


def level_of(key, dims, shards, smallest, largest):
    level = 1.0
    for position, shards_of in shards:
        steps = jax.random.uniform(jax.random.fold_in(jax.random.fold_in(key, 6), position), (shards_of,), jnp.float32, smallest / len(shards), largest / len(shards))
        level = level * jnp.repeat(jnp.exp(steps), dims[position] // shards_of).reshape((-1,) + (1,) * (len(dims) - 1 - position))
    return level


def normal_values(rng, extent, deviation, bound, cuts=(), kind=jnp.bfloat16):
    level = level_of(rng, extent, cuts, -0.22, 0.18) if cuts else 1.0
    drawn = jax.random.normal(rng, extent, jnp.float32) * deviation * level
    return jnp.minimum(jnp.maximum(drawn, -bound), bound).astype(kind)


def setup_inputs(seed: int = 0) -> dict:
    key_list = jax.random.split(jax.random.key(seed), 16)
    return {
        "mixer_input": normal_values(key_list[0], (TOKENS, D), 1.0, 6.0, ((0, 64),)),
        "mixer_gain": jnp.clip(1.0 + 0.18 * jax.random.normal(key_list[1], (D,), jnp.float32), 0.1, 1.9),
        "value_weight": normal_values(key_list[2], (D, CW), D ** -0.5, 0.125, ((1, 4),)),
        "inner_gate": normal_values(key_list[3], (D, CW), D ** -0.5, 0.125, ((1, 4),)),
        "outer_gate": normal_values(key_list[4], (D, CW), D ** -0.5, 0.125, ((1, 4),)),
        "kernel_taps": normal_values(key_list[5], (TAPS, CW), 0.6, 3.0, ((1, 4),), jnp.float32),
        "mixer_proj": normal_values(key_list[6], (CW, D), CW ** -0.5, 0.1875, ((0, 4),)),
        "expert_input": normal_values(key_list[7], (TOKENS, D), 1.0, 6.0, ((0, 256),)),
        "expert_gain": jnp.clip(1.0 + 0.18 * jax.random.normal(key_list[8], (D,), jnp.float32), 0.1, 1.9),
        "routes": draw_routes(jax.random.fold_in(key_list[15], 71), 0),
        "group_logits": normal_values(key_list[10], (TOKENS, GROUPS), 1.5, 6.0, ((0, 256),), jnp.float32),
        "pair_logits": normal_values(key_list[11], (TOKENS, 2), 1.5, 6.0, ((0, 256),), jnp.float32),
        "gate_weight": normal_values(key_list[12], (EXPERTS, D, FF), D ** -0.5, 0.125, ((0, 64), (2, 4))),
        "up_weight": normal_values(key_list[13], (EXPERTS, D, FF), D ** -0.5, 0.125, ((0, 64), (2, 4))),
        "down_weight": normal_values(key_list[14], (EXPERTS, FF, D), (FF // 16) ** -0.5, 0.75, ((0, 64), (1, 4))),
    }


EPSILON = 1e-06

def normed(values, gain):
    wide = values.astype(jnp.float32)
    scale = lax.rsqrt(lax.optimization_barrier(jnp.mean(wide * wide, axis=-1, keepdims=True)) + EPSILON)
    return (wide * scale * gain).astype(jnp.bfloat16)

def blockwise_sum(left, right, blocks):
    width = left.shape[1] // blocks
    total = jnp.zeros((left.shape[0], right.shape[1]), jnp.float32)
    for block in range(blocks):
        part = jnp.dot(left[:, block * width:(block + 1) * width], right[block * width:(block + 1) * width], preferred_element_type=jnp.float32)
        rounded = lax.optimization_barrier(part.astype(jnp.bfloat16))
        total = total + rounded.astype(jnp.float32)
    return total.astype(jnp.bfloat16)

def route_weights(routes, group_logits, pair_logits):
    chosen = routes[:, 0] // EPG
    groups = jnp.arange(group_logits.shape[1], dtype=jnp.int32)
    picked = lax.optimization_barrier(jnp.sum(jnp.where(groups[None, :] == chosen[:, None], group_logits, 0.0), axis=1))
    group_weight = 1.0 / lax.optimization_barrier(jnp.sum(jnp.exp(group_logits - picked[:, None]), axis=1))
    return group_weight[:, None] * jax.nn.sigmoid(pair_logits - pair_logits[:, ::-1])

def expert_block(rows, gate, upper, down, blocks):
    first = jnp.dot(rows, gate, preferred_element_type=jnp.float32)
    second = jnp.dot(rows, upper, preferred_element_type=jnp.float32)
    hidden = (jax.nn.silu(first) * second).astype(jnp.bfloat16)
    return blockwise_sum(hidden, down, blocks)

def reference(mixer_input, mixer_gain, value_weight, inner_gate, outer_gate, kernel_taps, mixer_proj, expert_input, expert_gain, routes, group_logits, pair_logits, gate_weight, up_weight, down_weight):
    normal_rows = normed(mixer_input, mixer_gain)
    values = jnp.dot(normal_rows, value_weight, preferred_element_type=jnp.float32)
    inner = jnp.dot(normal_rows, inner_gate, preferred_element_type=jnp.float32)
    outer = jnp.dot(normal_rows, outer_gate, preferred_element_type=jnp.float32)
    mixed_in = (inner * values).astype(jnp.bfloat16)
    padded = jnp.pad(mixed_in, ((1, 1), (0, 0))).astype(jnp.float32)
    conv_sum = kernel_taps[0] * padded[:-2] + kernel_taps[1] * padded[1:-1] + kernel_taps[2] * padded[2:]
    mixer_rows = (outer * conv_sum).astype(jnp.bfloat16)
    mixer_output = blockwise_sum(mixer_rows, mixer_proj, N_TP)
    expert_norm = normed(expert_input, expert_gain)
    weights = route_weights(routes, group_logits, pair_logits)
    flat = routes.reshape(-1)
    count = flat.shape[0]
    order = jnp.argsort(flat, stable=True).astype(jnp.int32)
    experts_iota = jnp.arange(EXPERTS, dtype=jnp.int32)
    loads = lax.optimization_barrier(jnp.sum((flat[:, None] == experts_iota[None, :]).astype(jnp.int32), axis=0))
    starts = (jnp.cumsum(loads) - loads).astype(jnp.int32)
    most = N_EP * N_TP * CAP
    padded_order = jnp.concatenate([order, jnp.full((most,), count, jnp.int32)])
    rows_pad = jnp.concatenate([expert_norm, jnp.zeros((1, D), jnp.bfloat16)])

    def one_expert(results, expert):
        picks = lax.dynamic_slice_in_dim(padded_order, starts[expert], most)
        live = jnp.arange(most, dtype=jnp.int32) < loads[expert]
        picks = jnp.where(live, picks, count).astype(jnp.int32)
        sources = jnp.where(live, picks // 2, count // 2).astype(jnp.int32)
        answers = expert_block(rows_pad[sources], gate_weight[expert], up_weight[expert], down_weight[expert], N_TP)
        return (results.at[picks].set(answers), None)
    results = jnp.zeros((count + 1, D), jnp.bfloat16)
    results, _ = lax.scan(one_expert, results, experts_iota)
    pairs = results[:count].reshape(count // 2, 2, D).astype(jnp.float32)
    expert_output = lax.optimization_barrier(jnp.sum(weights[:, :, None] * pairs, axis=1)).astype(jnp.bfloat16)
    return (mixer_output, expert_output)
```

```python
import jax
import jax.numpy as jnp
from jax import lax
from jax.sharding import PartitionSpec as P

EPG = 8
EPSILON = 1e-06


def padded_2(cells, axis):
    count = lax.axis_size(axis)
    ends = count - 1
    head = cells[:1]
    tail = cells[-1:]
    return jnp.concatenate(
        [
            lax.ppermute(tail, axis, [(i, i + 1) for i in range(ends)]),
            cells,
            lax.ppermute(head, axis, [(i + 1, i) for i in range(ends)]),
        ],
        axis=0,
    )


def normed(values, gain):
    wide = values.astype(jnp.float32)
    scale = lax.rsqrt(jnp.mean(wide * wide, axis=-1, keepdims=True) + EPSILON)
    return (wide * scale * gain).astype(jnp.bfloat16)


def route_weights(routes, group_logits, pair_logits):
    chosen = routes[:, 0] // EPG
    groups = jnp.arange(group_logits.shape[1], dtype=jnp.int32)
    picked = jnp.sum(jnp.where(groups[None, :] == chosen[:, None], group_logits, 0.0), axis=1)
    group_weight = 1.0 / jnp.sum(jnp.exp(group_logits - picked[:, None]), axis=1)
    return group_weight[:, None] * jax.nn.sigmoid(pair_logits - pair_logits[:, ::-1])


def f32dot(a, b):
    return jnp.dot(a, b, preferred_element_type=jnp.float32)


def on_device(
    mixer_input, mixer_gain, value_weight, inner_gate, outer_gate, kernel_taps, mixer_proj,
    expert_input, expert_gain, routes, group_logits, pair_logits, gate_weight, up_weight, down_weight,
):
    split = lax.axis_size("tp")
    experts = lax.axis_size("ep")
    n_groups = experts // EPG
    local = expert_input.shape[0]
    width = expert_input.shape[1]
    per = local // n_groups
    expert_norm = normed(expert_input, expert_gain)
    weights = route_weights(routes, group_logits, pair_logits)
    member = routes % EPG
    lanes = jnp.arange(EPG, dtype=jnp.int32)
    wide_w = (
        jnp.where(member[:, 0:1] == lanes, weights[:, 0:1], 0.0)
        + jnp.where(member[:, 1:2] == lanes, weights[:, 1:2], 0.0)
    )
    high = wide_w.astype(jnp.bfloat16)
    low = (wide_w - high.astype(jnp.float32)).astype(jnp.bfloat16)
    extra = jnp.concatenate([high, low, jnp.zeros((local, 128 - 2 * EPG), jnp.bfloat16)], axis=1)
    group = routes[:, 0] // EPG
    place = jnp.arange(local, dtype=jnp.int32)
    earlier = (group[:, None] == group[None, :]) & (place[None, :] < place[:, None])
    slot = group * per + jnp.sum(earlier.astype(jnp.int32), axis=1)
    onehot = (slot[:, None] == place[None, :]).astype(jnp.bfloat16)
    rows = jnp.concatenate([expert_norm, extra], axis=1)
    ordered = lax.dot_general(
        onehot, rows, (((0,), (0,)), ((), ())), preferred_element_type=jnp.float32
    ).astype(jnp.bfloat16)
    z_groups = [[z * EPG + i for z in range(n_groups)] for i in range(EPG)]
    plane_groups = [[z * EPG + i for i in range(EPG)] for z in range(n_groups)]
    arrived = lax.all_to_all(
        ordered, "ep", split_axis=0, concat_axis=0, axis_index_groups=z_groups, tiled=True
    )
    everyone = lax.all_gather(
        arrived, "ep", axis=0, axis_index_groups=plane_groups, tiled=True
    )
    all_gate = lax.all_gather(gate_weight[0], "tp", axis=0)
    all_up = lax.all_gather(up_weight[0], "tp", axis=0)
    all_down = lax.all_gather(down_weight[0], "tp", axis=0, tiled=True)

    normal_rows = normed(mixer_input, mixer_gain)
    values = f32dot(normal_rows, value_weight)
    inner = f32dot(normal_rows, inner_gate)
    outer = f32dot(normal_rows, outer_gate)
    mixed_in = (inner * values).astype(jnp.bfloat16)
    padded = padded_2(mixed_in, "ep").astype(jnp.float32)
    conv_sum = (
        kernel_taps[0] * padded[:-2] + kernel_taps[1] * padded[1:-1] + kernel_taps[2] * padded[2:]
    )
    mixer_rows = (outer * conv_sum).astype(jnp.bfloat16)
    partial = f32dot(mixer_rows, mixer_proj).astype(jnp.bfloat16)
    blocks = lax.all_to_all(partial.reshape(split, -1, width), "tp", 0, 0, tiled=True)
    mixer_output = jnp.sum(blocks.astype(jnp.float32), axis=0).astype(jnp.bfloat16)

    tokens = everyone[:, :width]
    mine = lax.axis_index("ep") % EPG
    both = everyone[:, width:].astype(jnp.float32)
    spot = jnp.arange(128, dtype=jnp.int32)
    weight = jnp.sum(jnp.where((spot == mine) | (spot == mine + EPG), both, 0.0), axis=1, keepdims=True)
    parts = []
    for j in range(split):
        first = f32dot(tokens, all_gate[j])
        second = f32dot(tokens, all_up[j])
        parts.append((jax.nn.silu(first) * second).astype(jnp.bfloat16))
    hidden = jnp.concatenate(parts, axis=1)
    answers = (f32dot(hidden, all_down) * weight).astype(jnp.bfloat16)
    home = lax.psum_scatter(
        answers, "ep", scatter_dimension=0, axis_index_groups=plane_groups, tiled=True
    )
    back = lax.all_to_all(
        home, "ep", split_axis=0, concat_axis=0, axis_index_groups=z_groups, tiled=True
    )
    expert_output = f32dot(onehot, back).astype(jnp.bfloat16)
    return (mixer_output, expert_output)


def solution(mesh):
    in_specs = (
        P("ep", None), P(), P(None, "tp"), P(None, "tp"), P(None, "tp"), P(None, "tp"), P("tp", None),
        P(("ep", "tp"), None), P(), P(("ep", "tp"), None), P(("ep", "tp"), None), P(("ep", "tp"), None),
        P("ep", None, "tp"), P("ep", None, "tp"), P("ep", "tp", None),
    )
    out_specs = (P(("ep", "tp"), None), P(("ep", "tp"), None))
    return jax.shard_map(
        on_device, mesh=mesh, in_specs=in_specs, out_specs=out_specs, check_vma=False
    )
```

```python
import jax
import jax.numpy as jnp
from jax import lax
from jax.experimental import pallas as pl
from jax.experimental.pallas import tpu as pltpu
from jax.sharding import PartitionSpec as P

MESH = pl.DeviceIdType.MESH
EPSILON = 1e-06
BF16 = jnp.bfloat16
F32 = jnp.float32
D = 2048
WIDE = D + 128
TOK = 160
HALF = 80
PER = 20
PAD = 32
GROUPS = 8
MEMBERS = 8
NX = 4
NY = 4
LOC = 256
CHUNKS = 4
CW = D // CHUNKS
COPIES = 128


def dot(a, b):
    return jnp.dot(a, b, preferred_element_type=F32)


def iota(shape, dim):
    return lax.broadcasted_iota(jnp.int32, shape, dim)


def scaled(wide, gain):
    mean = jnp.mean(wide * wide, axis=-1, keepdims=True)
    return (wide * lax.rsqrt(mean + EPSILON) * gain).astype(BF16)


def kernel(
    mixer_input, mixer_gain, value_weight, inner_gate, outer_gate, taps, mixer_proj,
    expert_input, expert_gain, routes, group_logits, pair_logits, gate_weight, up_weight, down_weight,
    mixer_output, expert_output,
    m_in, w_v, w_i, w_o, w_p, e_in, w_g, w_u, w_d,
    rows, z_out, z_in, tokens, hidden, mixed, outer, m_rows, m_parts, from_prev, from_next,
    m_a, m_b, m_p, m_n,
    parts, pair, r_a, r_b, r_p, r_n, home, zr_out, zr_in, spread, unsort,
    send_sems, recv_sems, local_sems,
):
    ep = lax.axis_index("ep")
    y = lax.axis_index("tp")
    core = lax.rem(ep, 2)
    x = lax.rem(ep // 2, NX)
    z = ep // MEMBERS
    n_ep = GROUPS * MEMBERS

    def at(zz, xx, cc):
        return zz * MEMBERS + xx * 2 + cc

    y_next = (ep, lax.rem(y + 1, NY))
    y_prev = (ep, lax.rem(y + NY - 1, NY))
    x_next = (at(z, lax.rem(x + 1, NX), core), y)
    x_prev = (at(z, lax.rem(x + NX - 1, NX), core), y)
    twin = (at(z, x, 1 - core), y)
    s_next = (lax.rem(ep + 1, n_ep), y)
    s_prev = (lax.rem(ep + n_ep - 1, n_ep), y)
    z_plus = [(at(lax.rem(z + d, GROUPS), x, core), y) for d in range(GROUPS)]
    z_minus = [(at(lax.rem(z + GROUPS - d, GROUPS), x, core), y) for d in range(GROUPS)]

    locals_ = []

    def load(src, dst):
        copy = pltpu.make_async_copy(src, dst, local_sems.at[len(locals_)])
        locals_.append(copy)
        copy.start()
        return copy

    copies = []

    def send(src, dst, device):
        k = len(copies)
        copy = pltpu.make_async_remote_copy(
            src_ref=src, dst_ref=dst, send_sem=send_sems.at[k], recv_sem=recv_sems.at[k],
            device_id=device, device_id_type=MESH,
        )
        copies.append(copy)
        copy.start()
        return copy

    l_ein = load(expert_input, e_in)
    l_min = load(mixer_input, m_in)
    l_v = load(value_weight, w_v)
    l_i = load(inner_gate, w_i)
    l_o = load(outer_gate, w_o)
    l_p = load(mixer_proj, w_p)
    l_g = load(gate_weight.at[0], w_g.at[0])
    l_u = load(up_weight.at[0], w_u.at[0])
    l_d = [
        load(down_weight.at[0, :, pl.ds(k * CW, CW)], w_d.at[k, pl.ds(0, LOC)]) for k in range(CHUNKS)
    ]

    barrier = pltpu.get_barrier_semaphore()
    partners = [y_next, y_prev, x_next, x_prev, twin, s_next, s_prev] + z_plus[1:]
    for device in partners:
        pl.semaphore_signal(barrier, inc=1, device_id=device, device_id_type=MESH)
    pl.semaphore_wait(barrier, len(partners))

    g_next = send(gate_weight.at[0], w_g.at[1], y_next)
    g_prev = send(gate_weight.at[0], w_g.at[3], y_prev)
    u_next = send(up_weight.at[0], w_u.at[1], y_next)
    u_prev = send(up_weight.at[0], w_u.at[3], y_prev)

    l_ein.wait()
    e_gain = expert_gain[...]

    def norm_expert(i, _):
        at_ = pl.ds(pl.multiple_of(i * 32, 32), 32)
        rows[at_, pl.ds(0, D)] = scaled(e_in[at_, :].astype(F32), e_gain)
        return 0

    lax.fori_loop(0, TOK // 32, norm_expert, 0)
    first = routes[:, 0:1]
    second = routes[:, 1:2]
    group = lax.shift_right_logical(first, 3)
    logits = group_logits[...]
    picked = jnp.sum(
        jnp.where(iota((TOK, GROUPS), 1) == group, logits, 0.0), axis=1, keepdims=True
    )
    g_weight = 1.0 / jnp.sum(jnp.exp(logits - picked), axis=1, keepdims=True)
    p0 = pair_logits[:, 0:1]
    p1 = pair_logits[:, 1:2]
    weight0 = g_weight / (1.0 + jnp.exp(p1 - p0))
    weight1 = g_weight / (1.0 + jnp.exp(p0 - p1))
    lane = iota((TOK, 128), 1)
    member = lax.bitwise_and(lane, 7)
    wide_w = jnp.where(member == lax.bitwise_and(first, 7), weight0, 0.0) + jnp.where(
        member == lax.bitwise_and(second, 7), weight1, 0.0
    )
    high = wide_w.astype(BF16).astype(F32)
    extra = jnp.where(lane < 8, high, jnp.where(lane < 16, wide_w - high, 0.0))
    rows[:, pl.ds(D, 128)] = extra.astype(BF16)

    rel = lax.bitwise_and(group + (GROUPS - z), 7).astype(F32)
    square = (TOK, TOK)
    sub, lan = iota(square, 0), iota(square, 1)
    rel_row = jnp.sum(jnp.where(sub == lan, rel, 0.0), axis=0, keepdims=True)
    same = rel == rel_row
    rank_col = jnp.sum(jnp.where(same & (lan < sub), 1.0, 0.0), axis=1, keepdims=True)
    rank_row = jnp.sum(jnp.where(same & (sub < lan), 1.0, 0.0), axis=0, keepdims=True)
    slot_col = (rel * PAD + rank_col).astype(jnp.int32)
    slot_row = (rel_row * PAD + rank_row).astype(jnp.int32)
    unsort[...] = (iota((TOK, GROUPS * PAD), 1) == slot_col).astype(F32).astype(BF16)
    sort = (iota((GROUPS * PAD, TOK), 0) == slot_row).astype(F32).astype(BF16)
    for q in range(4):
        cols = pl.ds(q * CW, CW)
        z_out[:, cols] = dot(sort, rows[:, cols]).astype(BF16)
    z_out[:, pl.ds(D, 128)] = dot(sort, rows[:, pl.ds(D, 128)]).astype(BF16)
    z_sent = [
        send(z_out.at[pl.ds(d * PAD, PAD)], z_in.at[pl.ds(d * PAD, PAD)], z_plus[d])
        for d in range(1, GROUPS)
    ]
    z_in[pl.ds(0, PAD), :] = z_out[pl.ds(0, PAD), :]

    m_gain = mixer_gain[...]
    for copy in (l_min, l_v, l_i, l_o):
        copy.wait()

    def norm_mixer(i, _):
        at_ = pl.ds(pl.multiple_of(i * 32, 32), 32)
        m_in[at_, :] = scaled(m_in[at_, :].astype(F32), m_gain)
        return 0

    lax.fori_loop(0, NY * TOK // 32, norm_mixer, 0)

    def gates(i, _):
        at_ = pl.ds(pl.multiple_of(i * TOK, TOK), TOK)
        block = m_in[at_, :]
        value = dot(block, w_v[...])
        inner = dot(block, w_i[...])
        mixed[pl.ds(pl.multiple_of(i * TOK + 8, 8), TOK), :] = (inner * value).astype(BF16).astype(F32)
        outer[at_, :] = dot(block, w_o[...])
        return 0

    lax.fori_loop(0, NY, gates, 0)
    h_next = send(mixed.at[pl.ds(NY * TOK, 8)], from_prev, s_next)
    h_prev = send(mixed.at[pl.ds(8, 8)], from_next, s_prev)
    l_p.wait()
    h_next.wait_recv()
    h_prev.wait_recv()
    mixed[pl.ds(7, 1), :] = jnp.where(ep == 0, 0.0, from_prev[pl.ds(7, 1), :])
    mixed[pl.ds(NY * TOK + 8, 1), :] = jnp.where(ep == n_ep - 1, 0.0, from_next[pl.ds(0, 1), :])
    t0, t1, t2 = taps[0:1, :], taps[1:2, :], taps[2:3, :]
    for i in range(NY):
        at_ = i * TOK
        conv = (
            t0 * mixed[pl.ds(at_ + 7, TOK), :]
            + t1 * mixed[pl.ds(at_ + 8, TOK), :]
            + t2 * mixed[pl.ds(at_ + 9, TOK), :]
        )
        m_rows[pl.ds(at_, TOK), :] = (outer[pl.ds(at_, TOK), :] * conv).astype(BF16)

    def project(i, _):
        r = i // 4
        cols = pl.ds(pl.multiple_of(lax.rem(i, 4) * CW, CW), CW)
        begin = pl.multiple_of(lax.rem(y + r, NY) * TOK, TOK)
        block = m_rows[pl.ds(begin, TOK), :]
        m_parts[pl.ds(pl.multiple_of(r * TOK, TOK), TOK), cols] = dot(block, w_p[:, cols]).astype(BF16)
        return 0

    lax.fori_loop(0, NY * 4, project, 0)

    g_next.wait_recv()
    f_g = send(w_g.at[1], w_g.at[2], y_next)

    for copy in z_sent:
        copy.wait_recv()
    p_sub = iota((TOK, GROUPS * PAD), 0)
    shift = jnp.zeros((TOK, GROUPS * PAD), jnp.int32)
    for d in range(1, GROUPS):
        shift = shift + jnp.where(p_sub >= d * PER, PAD - PER, 0)
    compact = (iota((TOK, GROUPS * PAD), 1) == p_sub + shift).astype(F32).astype(BF16)
    q_lan = iota((GROUPS * PAD, TOK), 1)
    shift = jnp.zeros((GROUPS * PAD, TOK), jnp.int32)
    for d in range(1, GROUPS):
        shift = shift + jnp.where(q_lan >= d * PER, PAD - PER, 0)
    spread[...] = (iota((GROUPS * PAD, TOK), 0) == q_lan + shift).astype(F32).astype(BF16)
    for q in range(4):
        cols = pl.ds(q * CW, CW)
        tokens[pl.ds(0, TOK), cols] = dot(compact, z_in[:, cols]).astype(BF16)
    tokens[pl.ds(0, TOK), pl.ds(D, 128)] = dot(compact, z_in[:, pl.ds(D, 128)]).astype(BF16)

    def block(b, h=None):
        if h is None:
            return tokens.at[pl.ds(b * TOK, TOK)]
        return tokens.at[pl.ds(b * TOK + h * HALF, HALF)]

    a_next = [None, None]
    a_prev = [None, None]
    a_next[0] = send(block(0, 0), block(1, 0), x_next)
    a_prev[1] = send(block(0, 1), block(3, 1), x_prev)
    a_next[1] = send(block(0, 1), block(1, 1), x_next)
    a_prev[0] = send(block(0, 0), block(3, 0), x_prev)
    c_own = send(block(0), block(4), twin)
    a_next[0].wait_recv()
    f_next = send(block(1, 0), block(2, 0), x_next)
    a_prev[1].wait_recv()
    f_prev = send(block(3, 1), block(2, 1), x_prev)
    a_next[1].wait_recv()
    c_1 = send(block(1), block(5), twin)
    a_prev[0].wait_recv()
    c_3 = send(block(3), block(7), twin)

    u_prev.wait_recv()
    f_u = send(w_u.at[3], w_u.at[2], y_prev)

    d_next = [None] * CHUNKS
    d_prev = [None] * CHUNKS

    def down_send(k):
        src = down_weight.at[0, :, pl.ds(k * CW, CW)]
        d_next[k] = send(src, w_d.at[k, pl.ds(LOC, LOC)], y_next)
        d_prev[k] = send(src, w_d.at[k, pl.ds(3 * LOC, LOC)], y_prev)

    down_send(0)
    down_send(1)

    f_next.wait_recv()
    f_prev.wait_recv()
    c_2 = send(block(2), block(6), twin)
    for copy in (c_own, c_1, c_3, c_2):
        copy.wait_recv()

    TILE = 320
    TILES = MEMBERS * TOK // TILE

    def ffn(j):
        def body(i, _):
            at_ = pl.ds(pl.multiple_of(i * TILE, TILE), TILE)
            block_ = tokens[at_, pl.ds(0, D)]
            a = dot(block_, w_g[j])
            b = dot(block_, w_u[j])
            hidden[at_, pl.ds(j * LOC, LOC)] = (a / (1.0 + jnp.exp(-a)) * b).astype(BF16)
            return 0

        lax.fori_loop(0, TILES, body, 0)

    l_g.wait()
    l_u.wait()
    ffn(0)
    u_next.wait_recv()
    ffn(1)
    g_prev.wait_recv()
    ffn(3)
    f_g.wait_recv()
    f_u.wait_recv()
    ffn(2)
    for copy in l_d:
        copy.wait()

    own = x * 2 + core
    fd_next = [None] * CHUNKS
    fd_prev = [None] * CHUNKS
    e_sent = [None] * CHUNKS
    ra = [None] * CHUNKS
    rb = [None] * CHUNKS
    n_a = [None] * CHUNKS
    n_b = [None] * CHUNKS
    p_a = [None] * CHUNKS
    p_b = [None] * CHUNKS
    z_back = [None] * CHUNKS
    HC = CW // 2

    def down_forward(k):
        d_next[k].wait_recv()
        d_prev[k].wait_recv()
        fd_next[k] = send(
            w_d.at[k, pl.ds(LOC, LOC), pl.ds(0, HC)], w_d.at[k, pl.ds(2 * LOC, LOC), pl.ds(0, HC)], y_next
        )
        fd_prev[k] = send(
            w_d.at[k, pl.ds(3 * LOC, LOC), pl.ds(HC, HC)], w_d.at[k, pl.ds(2 * LOC, LOC), pl.ds(HC, HC)], y_prev
        )

    def results(k):
        fd_next[k].wait_recv()
        fd_prev[k].wait_recv()

        def body(i, _):
            at_ = pl.ds(pl.multiple_of(i * TILE, TILE), TILE)
            both = tokens[at_, pl.ds(D, 128)].astype(F32)
            lane_ = iota((TILE, 128), 1)
            mine = (lane_ == own) | (lane_ == own + 8)
            weight = jnp.sum(jnp.where(mine, both, 0.0), axis=1, keepdims=True)
            parts[k, at_, :] = (dot(hidden[at_, :], w_d[k]) * weight).astype(BF16)
            return 0

        lax.fori_loop(0, TILES, body, 0)
        e_sent[k] = send(parts.at[k, pl.ds(NX * TOK, NX * TOK)], pair.at[k], twin)

    def add_into(ref, k, begin, count, other):
        at_ = pl.ds(begin, count)
        ref[k, at_, :] = (ref[k, at_, :].astype(F32) + other.astype(F32)).astype(BF16)

    def merge(k):
        e_sent[k].wait_recv()
        for rx in (2, 3, 1, 0):
            add_into(parts, k, rx * TOK, TOK, pair[k, pl.ds(rx * TOK, TOK), :])
        rb[k] = send(parts.at[k, pl.ds(2 * TOK + HALF, HALF)], r_b.at[k], x_next)
        ra[k] = send(parts.at[k, pl.ds(2 * TOK, HALF)], r_a.at[k], x_prev)
        n_a[k] = send(parts.at[k, pl.ds(3 * TOK, HALF)], r_p.at[k, pl.ds(0, HALF)], x_next)
        p_b[k] = send(parts.at[k, pl.ds(TOK + HALF, HALF)], r_n.at[k, pl.ds(HALF, HALF)], x_prev)

    def relay(k):
        rb[k].wait_recv()
        add_into(parts, k, 3 * TOK + HALF, HALF, r_b[k])
        n_b[k] = send(parts.at[k, pl.ds(3 * TOK + HALF, HALF)], r_p.at[k, pl.ds(HALF, HALF)], x_next)
        ra[k].wait_recv()
        add_into(parts, k, TOK, HALF, r_a[k])
        p_a[k] = send(parts.at[k, pl.ds(TOK, HALF)], r_n.at[k, pl.ds(0, HALF)], x_prev)

    def arrive(k):
        for copy in (n_a[k], p_b[k], n_b[k], p_a[k]):
            copy.wait_recv()
        total = (
            parts[k, pl.ds(0, TOK), :].astype(F32) + r_p[k].astype(F32) + r_n[k].astype(F32)
        ).astype(BF16)
        zr_out[k] = dot(spread[...], total).astype(BF16)
        z_back[k] = [
            send(zr_out.at[k, pl.ds(d * PAD, PAD)], zr_in.at[k, pl.ds(d * PAD, PAD)], z_minus[d])
            for d in range(1, GROUPS)
        ]
        zr_in[k, pl.ds(0, PAD), :] = zr_out[k, pl.ds(0, PAD), :]

    def finish(k):
        for copy in z_back[k]:
            copy.wait_recv()
        expert_output[:, pl.ds(k * CW, CW)] = dot(unsort[...], zr_in[k]).astype(BF16)

    def m_add(begin, other):
        def body(i, _):
            cols = pl.ds(pl.multiple_of(i * CW, CW), CW)
            at_ = pl.ds(begin, HALF)
            m_parts[at_, cols] = (m_parts[at_, cols].astype(F32) + other[:, cols].astype(F32)).astype(BF16)
            return 0

        lax.fori_loop(0, 4, body, 0)

    down_forward(0)
    down_send(2)
    down_forward(1)
    down_send(3)
    results(0)
    down_forward(2)
    merge(0)
    results(1)
    relay(0)
    merge(1)
    down_forward(3)
    mb = send(m_parts.at[pl.ds(2 * TOK + HALF, HALF)], m_b, y_next)
    ma = send(m_parts.at[pl.ds(2 * TOK, HALF)], m_a, y_prev)
    mn_a = send(m_parts.at[pl.ds(TOK, HALF)], m_p.at[pl.ds(0, HALF)], y_next)
    mp_b = send(m_parts.at[pl.ds(3 * TOK + HALF, HALF)], m_n.at[pl.ds(HALF, HALF)], y_prev)
    arrive(0)
    relay(1)
    results(2)
    arrive(1)
    results(3)
    merge(2)
    merge(3)
    finish(0)
    relay(2)
    relay(3)
    mb.wait_recv()
    m_add(TOK + HALF, m_b)
    mn_b = send(m_parts.at[pl.ds(TOK + HALF, HALF)], m_p.at[pl.ds(HALF, HALF)], y_next)
    ma.wait_recv()
    m_add(3 * TOK, m_a)
    mp_a = send(m_parts.at[pl.ds(3 * TOK, HALF)], m_n.at[pl.ds(0, HALF)], y_prev)
    arrive(2)
    arrive(3)
    finish(1)
    finish(2)
    finish(3)
    for copy in (mn_a, mp_b, mn_b, mp_a):
        copy.wait_recv()

    def m_final(i, _):
        cols = pl.ds(pl.multiple_of(i * CW, CW), CW)
        mixer_output[:, cols] = (
            m_parts[pl.ds(0, TOK), cols].astype(F32) + m_p[:, cols].astype(F32) + m_n[:, cols].astype(F32)
        ).astype(BF16)
        return 0

    lax.fori_loop(0, 4, m_final, 0)
    for copy in copies:
        copy.wait_send()


def on_device(*args):
    args = list(args)
    args[1] = args[1].reshape(1, D)
    args[8] = args[8].reshape(1, D)
    any_ = pl.BlockSpec(memory_space=pl.ANY)
    vmem = pl.BlockSpec(memory_space=pltpu.VMEM)
    big = (0, 2, 3, 4, 6, 7, 12, 13, 14)
    out = jax.ShapeDtypeStruct((TOK, D), BF16)
    rows = MEMBERS * TOK
    scratch = [
        pltpu.VMEM((NY * TOK, D), BF16),
        pltpu.VMEM((D, LOC), BF16),
        pltpu.VMEM((D, LOC), BF16),
        pltpu.VMEM((D, LOC), BF16),
        pltpu.VMEM((LOC, D), BF16),
        pltpu.VMEM((TOK, D), BF16),
        pltpu.VMEM((NY, D, LOC), BF16),
        pltpu.VMEM((NY, D, LOC), BF16),
        pltpu.VMEM((CHUNKS, NY * LOC, CW), BF16),
        pltpu.VMEM((TOK, WIDE), BF16),
        pltpu.VMEM((GROUPS * PAD, WIDE), BF16),
        pltpu.VMEM((GROUPS * PAD, WIDE), BF16),
        pltpu.VMEM((rows, WIDE), BF16),
        pltpu.VMEM((rows, NY * LOC), BF16),
        pltpu.VMEM((NY * TOK + 16, LOC), F32),
        pltpu.VMEM((NY * TOK, LOC), F32),
        pltpu.VMEM((NY * TOK, LOC), BF16),
        pltpu.VMEM((NY * TOK, D), BF16),
        pltpu.VMEM((8, LOC), F32),
        pltpu.VMEM((8, LOC), F32),
        pltpu.VMEM((HALF, D), BF16),
        pltpu.VMEM((HALF, D), BF16),
        pltpu.VMEM((TOK, D), BF16),
        pltpu.VMEM((TOK, D), BF16),
        pltpu.VMEM((CHUNKS, rows, CW), BF16),
        pltpu.VMEM((CHUNKS, NX * TOK, CW), BF16),
        pltpu.VMEM((CHUNKS, HALF, CW), BF16),
        pltpu.VMEM((CHUNKS, HALF, CW), BF16),
        pltpu.VMEM((CHUNKS, TOK, CW), BF16),
        pltpu.VMEM((CHUNKS, TOK, CW), BF16),
        pltpu.VMEM((8, 128), F32),
        pltpu.VMEM((CHUNKS, GROUPS * PAD, CW), BF16),
        pltpu.VMEM((CHUNKS, GROUPS * PAD, CW), BF16),
        pltpu.VMEM((GROUPS * PAD, TOK), BF16),
        pltpu.VMEM((TOK, GROUPS * PAD), BF16),
        pltpu.SemaphoreType.DMA((COPIES,)),
        pltpu.SemaphoreType.DMA((COPIES,)),
        pltpu.SemaphoreType.DMA((16,)),
    ]
    return pl.pallas_call(
        kernel,
        out_shape=(out, out),
        in_specs=[any_ if k in big else vmem for k in range(15)],
        out_specs=(vmem, vmem),
        scratch_shapes=scratch,
        compiler_params=pltpu.CompilerParams(
            collective_id=0, has_side_effects=True, vmem_limit_bytes=67043328
        ),
        name="mixer_and_experts",
    )(*args)


def solution(mesh):
    in_specs = (
        P("ep", None), P(), P(None, "tp"), P(None, "tp"), P(None, "tp"), P(None, "tp"), P("tp", None),
        P(("ep", "tp"), None), P(), P(("ep", "tp"), None), P(("ep", "tp"), None), P(("ep", "tp"), None),
        P("ep", None, "tp"), P("ep", None, "tp"), P("ep", "tp", None),
    )
    out_specs = (P(("ep", "tp"), None), P(("ep", "tp"), None))
    return jax.shard_map(
        on_device, mesh=mesh, in_specs=in_specs, out_specs=out_specs, check_vma=False
    )
```

```python
import jax
import jax.numpy as jnp
from jax import lax
from jax.experimental import pallas as pl
from jax.experimental.pallas import tpu as pltpu
from jax.sharding import PartitionSpec as P

MESH = pl.DeviceIdType.MESH
EPSILON = 1e-06
BF16 = jnp.bfloat16
F32 = jnp.float32
D = 2048
WIDE = D + 128
TOK = 160
HALF = 80
PER = 20
PAD = 32
GROUPS = 8
MEMBERS = 8
NX = 4
NY = 4
LOC = 256
CHUNKS = 4
CW = D // CHUNKS
COPIES = 128


def dot(a, b):
    return jnp.dot(a, b, preferred_element_type=F32)


def iota(shape, dim):
    return lax.broadcasted_iota(jnp.int32, shape, dim)


def scaled(wide, gain):
    mean = jnp.mean(wide * wide, axis=-1, keepdims=True)
    return (wide * lax.rsqrt(mean + EPSILON) * gain).astype(BF16)


def kernel(
    mixer_input, mixer_gain, value_weight, inner_gate, outer_gate, taps, mixer_proj,
    expert_input, expert_gain, routes, group_logits, pair_logits, gate_weight, up_weight, down_weight,
    mixer_output, expert_output,
    m_in, w_v, w_i, w_o, w_p, e_in, w_g, w_u, w_d,
    rows, z_out, z_in, tokens, hidden, mixed, outer, m_rows, m_parts, from_prev, from_next,
    m_a, m_b, m_p, m_n,
    parts, pair, r_a, r_b, r_p, r_n, zr_out, zr_in, spread, unsort,
    send_sems, recv_sems, local_sems,
):
    ep = lax.axis_index("ep")
    y = lax.axis_index("tp")
    core = lax.rem(ep, 2)
    x = lax.rem(ep // 2, NX)
    z = ep // MEMBERS
    n_ep = GROUPS * MEMBERS

    def at(zz, xx, cc):
        return zz * MEMBERS + xx * 2 + cc

    y_next = (ep, lax.rem(y + 1, NY))
    y_prev = (ep, lax.rem(y + NY - 1, NY))
    x_next = (at(z, lax.rem(x + 1, NX), core), y)
    x_prev = (at(z, lax.rem(x + NX - 1, NX), core), y)
    twin = (at(z, x, 1 - core), y)
    s_next = (lax.rem(ep + 1, n_ep), y)
    s_prev = (lax.rem(ep + n_ep - 1, n_ep), y)
    z_plus = [(at(lax.rem(z + d, GROUPS), x, core), y) for d in range(GROUPS)]
    z_minus = [(at(lax.rem(z + GROUPS - d, GROUPS), x, core), y) for d in range(GROUPS)]

    locals_ = []

    def load(src, dst):
        copy = pltpu.make_async_copy(src, dst, local_sems.at[len(locals_)])
        locals_.append(copy)
        copy.start()
        return copy

    copies = []

    def send(src, dst, device):
        k = len(copies)
        copy = pltpu.make_async_remote_copy(
            src_ref=src, dst_ref=dst, send_sem=send_sems.at[k], recv_sem=recv_sems.at[k],
            device_id=device, device_id_type=MESH,
        )
        copies.append(copy)
        copy.start()
        return copy

    l_ein = load(expert_input, e_in)
    l_min = load(mixer_input, m_in)
    l_v = load(value_weight, w_v)
    l_i = load(inner_gate, w_i)
    l_o = load(outer_gate, w_o)
    l_p = load(mixer_proj, w_p)
    l_g = load(gate_weight.at[0], w_g.at[0])
    l_u = load(up_weight.at[0], w_u.at[0])
    l_d = [
        load(down_weight.at[0, :, pl.ds(k * CW, CW)], w_d.at[k, pl.ds(0, LOC)]) for k in range(CHUNKS)
    ]

    barrier = pltpu.get_barrier_semaphore()
    partners = [y_next, y_prev, x_next, x_prev, twin, s_next, s_prev] + z_plus[1:]
    for device in partners:
        pl.semaphore_signal(barrier, inc=1, device_id=device, device_id_type=MESH)
    pl.semaphore_wait(barrier, len(partners))

    g_next = send(gate_weight.at[0], w_g.at[1], y_next)
    g_prev = send(gate_weight.at[0], w_g.at[3], y_prev)
    u_next = send(up_weight.at[0], w_u.at[1], y_next)
    u_prev = send(up_weight.at[0], w_u.at[3], y_prev)

    d_next = [None] * CHUNKS
    d_prev = [None] * CHUNKS

    def down_send(k):
        src = down_weight.at[0, :, pl.ds(k * CW, CW)]
        d_next[k] = send(src, w_d.at[k, pl.ds(LOC, LOC)], y_next)
        d_prev[k] = send(src, w_d.at[k, pl.ds(3 * LOC, LOC)], y_prev)

    down_send(0)

    fd_next = [None] * CHUNKS
    fd_prev = [None] * CHUNKS
    HC = CW // 2

    def down_forward(k):
        d_next[k].wait_recv()
        d_prev[k].wait_recv()
        fd_next[k] = send(
            w_d.at[k, pl.ds(LOC, LOC), pl.ds(0, HC)], w_d.at[k, pl.ds(2 * LOC, LOC), pl.ds(0, HC)], y_next
        )
        fd_prev[k] = send(
            w_d.at[k, pl.ds(3 * LOC, LOC), pl.ds(HC, HC)], w_d.at[k, pl.ds(2 * LOC, LOC), pl.ds(HC, HC)], y_prev
        )

    l_ein.wait()
    e_gain = expert_gain[...]

    def norm_expert(i, _):
        at_ = pl.ds(pl.multiple_of(i * 32, 32), 32)
        rows[at_, pl.ds(0, D)] = scaled(e_in[at_, :].astype(F32), e_gain)
        return 0

    lax.fori_loop(0, TOK // 32, norm_expert, 0)
    first = routes[0:1, :]
    second = routes[1:2, :]
    group = lax.shift_right_logical(first, 3)
    logits = group_logits[...]
    picked = jnp.sum(jnp.where(iota((GROUPS, TOK), 0) == group, logits, 0.0), axis=0, keepdims=True)
    g_weight = 1.0 / jnp.sum(jnp.exp(logits - picked), axis=0, keepdims=True)
    p0 = pair_logits[0:1, :]
    p1 = pair_logits[1:2, :]
    weight0 = g_weight / (1.0 + jnp.exp(p1 - p0))
    weight1 = g_weight / (1.0 + jnp.exp(p0 - p1))
    line = iota((128, TOK), 0)
    member = lax.bitwise_and(line, 7)
    wide_w = jnp.where(member == lax.bitwise_and(first, 7), weight0, 0.0) + jnp.where(
        member == lax.bitwise_and(second, 7), weight1, 0.0
    )
    high = wide_w.astype(BF16).astype(F32)
    extra = jnp.where(line < 8, high, jnp.where(line < 16, wide_w - high, 0.0)).astype(BF16)

    rel_row = lax.bitwise_and(group + (GROUPS - z), 7).astype(F32)
    square = (TOK, TOK)
    sub, lan = iota(square, 0), iota(square, 1)
    rel_col = jnp.sum(jnp.where(sub == lan, rel_row, 0.0), axis=1, keepdims=True)
    earlier = (rel_col == rel_row) & (sub < lan)
    slot_row = rel_row * PAD + jnp.sum(jnp.where(earlier, 1.0, 0.0), axis=0, keepdims=True)
    slot_col = jnp.sum(jnp.where(sub == lan, slot_row, 0.0), axis=1, keepdims=True).astype(jnp.int32)
    slot_row = slot_row.astype(jnp.int32)
    sort = (iota((GROUPS * PAD, TOK), 0) == slot_row).astype(F32).astype(BF16)
    for q in range(4):
        cols = pl.ds(q * CW, CW)
        z_out[:, cols] = dot(sort, rows[:, cols]).astype(BF16)
    z_out[:, pl.ds(D, 128)] = lax.dot_general(
        sort, extra, (((1,), (1,)), ((), ())), preferred_element_type=F32
    ).astype(BF16)
    z_sent = [
        send(z_out.at[pl.ds(d * PAD, PAD)], z_in.at[pl.ds(d * PAD, PAD)], z_plus[d])
        for d in range(1, GROUPS)
    ]
    z_in[pl.ds(0, PAD), :] = z_out[pl.ds(0, PAD), :]
    unsort[...] = (iota((TOK, GROUPS * PAD), 1) == slot_col).astype(F32).astype(BF16)

    m_gain = mixer_gain[...]
    for copy in (l_min, l_v, l_i, l_o):
        copy.wait()

    def norm_mixer(i, _):
        at_ = pl.ds(pl.multiple_of(i * 32, 32), 32)
        m_in[at_, :] = scaled(m_in[at_, :].astype(F32), m_gain)
        return 0

    lax.fori_loop(0, NY * TOK // 32, norm_mixer, 0)

    def gates(i, _):
        at_ = pl.ds(pl.multiple_of(i * TOK, TOK), TOK)
        block = m_in[at_, :]
        value = dot(block, w_v[...])
        inner = dot(block, w_i[...])
        mixed[pl.ds(pl.multiple_of(i * TOK + 8, 8), TOK), :] = (inner * value).astype(BF16).astype(F32)
        outer[at_, :] = dot(block, w_o[...])
        return 0

    lax.fori_loop(0, NY, gates, 0)
    h_next = send(mixed.at[pl.ds(NY * TOK, 8)], from_prev, s_next)
    h_prev = send(mixed.at[pl.ds(8, 8)], from_next, s_prev)
    l_p.wait()
    h_next.wait_recv()
    h_prev.wait_recv()
    mixed[pl.ds(7, 1), :] = jnp.where(ep == 0, 0.0, from_prev[pl.ds(7, 1), :])
    mixed[pl.ds(NY * TOK + 8, 1), :] = jnp.where(ep == n_ep - 1, 0.0, from_next[pl.ds(0, 1), :])
    t0, t1, t2 = taps[0:1, :], taps[1:2, :], taps[2:3, :]
    for i in range(NY):
        at_ = i * TOK
        conv = (
            t0 * mixed[pl.ds(at_ + 7, TOK), :]
            + t1 * mixed[pl.ds(at_ + 8, TOK), :]
            + t2 * mixed[pl.ds(at_ + 9, TOK), :]
        )
        m_rows[pl.ds(at_, TOK), :] = (outer[pl.ds(at_, TOK), :] * conv).astype(BF16)

    def project(i, _):
        r = i // 4
        cols = pl.ds(pl.multiple_of(lax.rem(i, 4) * CW, CW), CW)
        begin = pl.multiple_of(lax.rem(y + r, NY) * TOK, TOK)
        block = m_rows[pl.ds(begin, TOK), :]
        m_parts[pl.ds(pl.multiple_of(r * TOK, TOK), TOK), cols] = dot(block, w_p[:, cols]).astype(BF16)
        return 0

    lax.fori_loop(0, NY * 4, project, 0)

    g_next.wait_recv()
    f_g = send(w_g.at[1], w_g.at[2], y_next)

    for copy in z_sent:
        copy.wait_recv()
    p_sub = iota((TOK, GROUPS * PAD), 0)
    shift = jnp.zeros((TOK, GROUPS * PAD), jnp.int32)
    for d in range(1, GROUPS):
        shift = shift + jnp.where(p_sub >= d * PER, PAD - PER, 0)
    compact = (iota((TOK, GROUPS * PAD), 1) == p_sub + shift).astype(F32).astype(BF16)
    q_lan = iota((GROUPS * PAD, TOK), 1)
    shift = jnp.zeros((GROUPS * PAD, TOK), jnp.int32)
    for d in range(1, GROUPS):
        shift = shift + jnp.where(q_lan >= d * PER, PAD - PER, 0)
    spread[...] = (iota((GROUPS * PAD, TOK), 0) == q_lan + shift).astype(F32).astype(BF16)
    for q in range(4):
        cols = pl.ds(q * CW, CW)
        tokens[pl.ds(0, TOK), cols] = dot(compact, z_in[:, cols]).astype(BF16)
    tokens[pl.ds(0, TOK), pl.ds(D, 128)] = dot(compact, z_in[:, pl.ds(D, 128)]).astype(BF16)

    def block(b, h=None):
        if h is None:
            return tokens.at[pl.ds(b * TOK, TOK)]
        return tokens.at[pl.ds(b * TOK + h * HALF, HALF)]

    a_next = [None, None]
    a_prev = [None, None]
    a_next[0] = send(block(0, 0), block(1, 0), x_next)
    a_prev[1] = send(block(0, 1), block(3, 1), x_prev)
    a_next[1] = send(block(0, 1), block(1, 1), x_next)
    a_prev[0] = send(block(0, 0), block(3, 0), x_prev)
    c_own = send(block(0), block(4), twin)
    a_next[0].wait_recv()
    f_next = send(block(1, 0), block(2, 0), x_next)
    a_prev[1].wait_recv()
    f_prev = send(block(3, 1), block(2, 1), x_prev)
    u_prev.wait_recv()
    f_u = send(w_u.at[3], w_u.at[2], y_prev)
    down_send(1)
    down_forward(0)
    down_send(2)
    a_next[1].wait_recv()
    c_1 = send(block(1), block(5), twin)
    a_prev[0].wait_recv()
    c_3 = send(block(3), block(7), twin)

    f_next.wait_recv()
    f_prev.wait_recv()
    c_2 = send(block(2), block(6), twin)
    for copy in (c_own, c_1, c_3, c_2):
        copy.wait_recv()

    TILE = 320
    TILES = MEMBERS * TOK // TILE

    def ffn(j):
        def body(i, _):
            at_ = pl.ds(pl.multiple_of(i * TILE, TILE), TILE)
            block_ = tokens[at_, pl.ds(0, D)]
            a = dot(block_, w_g[j])
            b = dot(block_, w_u[j])
            hidden[at_, pl.ds(j * LOC, LOC)] = (a / (1.0 + jnp.exp(-a)) * b).astype(BF16)
            return 0

        lax.fori_loop(0, TILES, body, 0)

    l_g.wait()
    l_u.wait()
    ffn(0)
    u_next.wait_recv()
    ffn(1)
    g_prev.wait_recv()
    ffn(3)
    f_g.wait_recv()
    f_u.wait_recv()
    ffn(2)
    for copy in l_d:
        copy.wait()

    own = x * 2 + core
    e_sent = [None] * CHUNKS
    ra = [None] * CHUNKS
    rb = [None] * CHUNKS
    n_a = [None] * CHUNKS
    n_b = [None] * CHUNKS
    p_a = [None] * CHUNKS
    p_b = [None] * CHUNKS
    z_back = [None] * CHUNKS

    def results(k):
        fd_next[k].wait_recv()
        fd_prev[k].wait_recv()

        def body(i, _):
            at_ = pl.ds(pl.multiple_of(i * TILE, TILE), TILE)
            both = tokens[at_, pl.ds(D, 128)].astype(F32)
            lane_ = iota((TILE, 128), 1)
            mine = (lane_ == own) | (lane_ == own + 8)
            weight = jnp.sum(jnp.where(mine, both, 0.0), axis=1, keepdims=True)
            parts[k, at_, :] = (dot(hidden[at_, :], w_d[k]) * weight).astype(BF16)
            return 0

        lax.fori_loop(0, TILES, body, 0)
        e_sent[k] = send(parts.at[k, pl.ds(NX * TOK, NX * TOK)], pair.at[k], twin)

    def add_into(ref, k, begin, count, other):
        at_ = pl.ds(begin, count)
        ref[k, at_, :] = (ref[k, at_, :].astype(F32) + other.astype(F32)).astype(BF16)

    def merge(k):
        e_sent[k].wait_recv()
        for rx in (2, 3, 1, 0):
            add_into(parts, k, rx * TOK, TOK, pair[k, pl.ds(rx * TOK, TOK), :])
        rb[k] = send(parts.at[k, pl.ds(2 * TOK + HALF, HALF)], r_b.at[k], x_next)
        ra[k] = send(parts.at[k, pl.ds(2 * TOK, HALF)], r_a.at[k], x_prev)
        n_a[k] = send(parts.at[k, pl.ds(3 * TOK, HALF)], r_p.at[k, pl.ds(0, HALF)], x_next)
        p_b[k] = send(parts.at[k, pl.ds(TOK + HALF, HALF)], r_n.at[k, pl.ds(HALF, HALF)], x_prev)

    def relay(k):
        rb[k].wait_recv()
        add_into(parts, k, 3 * TOK + HALF, HALF, r_b[k])
        n_b[k] = send(parts.at[k, pl.ds(3 * TOK + HALF, HALF)], r_p.at[k, pl.ds(HALF, HALF)], x_next)
        ra[k].wait_recv()
        add_into(parts, k, TOK, HALF, r_a[k])
        p_a[k] = send(parts.at[k, pl.ds(TOK, HALF)], r_n.at[k, pl.ds(0, HALF)], x_prev)

    def arrive(k):
        for copy in (n_a[k], p_b[k], n_b[k], p_a[k]):
            copy.wait_recv()
        total = (
            parts[k, pl.ds(0, TOK), :].astype(F32) + r_p[k].astype(F32) + r_n[k].astype(F32)
        ).astype(BF16)
        zr_out[k] = dot(spread[...], total).astype(BF16)
        z_back[k] = [
            send(zr_out.at[k, pl.ds(d * PAD, PAD)], zr_in.at[k, pl.ds(d * PAD, PAD)], z_minus[d])
            for d in range(1, GROUPS)
        ]
        zr_in[k, pl.ds(0, PAD), :] = zr_out[k, pl.ds(0, PAD), :]

    def finish(k):
        for copy in z_back[k]:
            copy.wait_recv()
        expert_output[:, pl.ds(k * CW, CW)] = dot(unsort[...], zr_in[k]).astype(BF16)

    def m_add(begin, other):
        def body(i, _):
            cols = pl.ds(pl.multiple_of(i * CW, CW), CW)
            at_ = pl.ds(begin, HALF)
            m_parts[at_, cols] = (m_parts[at_, cols].astype(F32) + other[:, cols].astype(F32)).astype(BF16)
            return 0

        lax.fori_loop(0, 4, body, 0)

    down_forward(1)
    down_send(3)
    results(0)
    down_forward(2)
    merge(0)
    results(1)
    relay(0)
    merge(1)
    down_forward(3)
    mb = send(m_parts.at[pl.ds(2 * TOK + HALF, HALF)], m_b, y_next)
    ma = send(m_parts.at[pl.ds(2 * TOK, HALF)], m_a, y_prev)
    mn_a = send(m_parts.at[pl.ds(TOK, HALF)], m_p.at[pl.ds(0, HALF)], y_next)
    mp_b = send(m_parts.at[pl.ds(3 * TOK + HALF, HALF)], m_n.at[pl.ds(HALF, HALF)], y_prev)
    arrive(0)
    relay(1)
    results(2)
    arrive(1)
    results(3)
    merge(2)
    merge(3)
    finish(0)
    relay(2)
    relay(3)
    mb.wait_recv()
    m_add(TOK + HALF, m_b)
    mn_b = send(m_parts.at[pl.ds(TOK + HALF, HALF)], m_p.at[pl.ds(HALF, HALF)], y_next)
    ma.wait_recv()
    m_add(3 * TOK, m_a)
    mp_a = send(m_parts.at[pl.ds(3 * TOK, HALF)], m_n.at[pl.ds(0, HALF)], y_prev)
    arrive(2)
    arrive(3)
    finish(1)
    finish(2)
    finish(3)
    for copy in (mn_a, mp_b, mn_b, mp_a):
        copy.wait_recv()

    def m_final(i, _):
        cols = pl.ds(pl.multiple_of(i * CW, CW), CW)
        mixer_output[:, cols] = (
            m_parts[pl.ds(0, TOK), cols].astype(F32) + m_p[:, cols].astype(F32) + m_n[:, cols].astype(F32)
        ).astype(BF16)
        return 0

    lax.fori_loop(0, 4, m_final, 0)
    for copy in copies:
        copy.wait_send()


def deliver(a, b, a_out, b_out, held, sems):
    loads = [pltpu.make_async_copy(r, held.at[k], sems.at[k]) for k, r in enumerate((a, b))]
    stores = [pltpu.make_async_copy(held.at[k], r, sems.at[k + 2]) for k, r in enumerate((a_out, b_out))]
    for copy in loads:
        copy.start()
    for copy, store in zip(loads, stores):
        copy.wait()
        store.start()
    for store in stores:
        store.wait()


def on_device(*args):
    args = list(args)
    args[1] = args[1].reshape(1, D)
    args[8] = args[8].reshape(1, D)
    for k in (9, 10, 11):
        args[k] = args[k].T
    any_ = pl.BlockSpec(memory_space=pl.ANY)
    vmem = pl.BlockSpec(memory_space=pltpu.VMEM)
    big = (0, 2, 3, 4, 6, 7, 12, 13, 14)
    out = jax.ShapeDtypeStruct((TOK, D), BF16)
    rows = MEMBERS * TOK
    scratch = [
        pltpu.VMEM((NY * TOK, D), BF16),
        pltpu.VMEM((D, LOC), BF16),
        pltpu.VMEM((D, LOC), BF16),
        pltpu.VMEM((D, LOC), BF16),
        pltpu.VMEM((LOC, D), BF16),
        pltpu.VMEM((TOK, D), BF16),
        pltpu.VMEM((NY, D, LOC), BF16),
        pltpu.VMEM((NY, D, LOC), BF16),
        pltpu.VMEM((CHUNKS, NY * LOC, CW), BF16),
        pltpu.VMEM((TOK, D), BF16),
        pltpu.VMEM((GROUPS * PAD, WIDE), BF16),
        pltpu.VMEM((GROUPS * PAD, WIDE), BF16),
        pltpu.VMEM((rows, WIDE), BF16),
        pltpu.VMEM((rows, NY * LOC), BF16),
        pltpu.VMEM((NY * TOK + 16, LOC), F32),
        pltpu.VMEM((NY * TOK, LOC), F32),
        pltpu.VMEM((NY * TOK, LOC), BF16),
        pltpu.VMEM((NY * TOK, D), BF16),
        pltpu.VMEM((8, LOC), F32),
        pltpu.VMEM((8, LOC), F32),
        pltpu.VMEM((HALF, D), BF16),
        pltpu.VMEM((HALF, D), BF16),
        pltpu.VMEM((TOK, D), BF16),
        pltpu.VMEM((TOK, D), BF16),
        pltpu.VMEM((CHUNKS, rows, CW), BF16),
        pltpu.VMEM((CHUNKS, NX * TOK, CW), BF16),
        pltpu.VMEM((CHUNKS, HALF, CW), BF16),
        pltpu.VMEM((CHUNKS, HALF, CW), BF16),
        pltpu.VMEM((CHUNKS, TOK, CW), BF16),
        pltpu.VMEM((CHUNKS, TOK, CW), BF16),
        pltpu.VMEM((CHUNKS, GROUPS * PAD, CW), BF16),
        pltpu.VMEM((CHUNKS, GROUPS * PAD, CW), BF16),
        pltpu.VMEM((GROUPS * PAD, TOK), BF16),
        pltpu.VMEM((TOK, GROUPS * PAD), BF16),
        pltpu.SemaphoreType.DMA((COPIES,)),
        pltpu.SemaphoreType.DMA((COPIES,)),
        pltpu.SemaphoreType.DMA((16,)),
    ]
    results = pl.pallas_call(
        kernel,
        out_shape=(out, out),
        in_specs=[any_ if k in big else vmem for k in range(15)],
        out_specs=(vmem, vmem),
        scratch_shapes=scratch,
        compiler_params=pltpu.CompilerParams(
            collective_id=0, has_side_effects=True, vmem_limit_bytes=67043328
        ),
        name="mixer_and_experts",
    )(*args)
    return pl.pallas_call(
        deliver,
        out_shape=(out, out),
        in_specs=[any_, any_],
        out_specs=(any_, any_),
        scratch_shapes=[pltpu.VMEM((2, TOK, D), BF16), pltpu.SemaphoreType.DMA((4,))],
        name="deliver",
    )(*results)


def solution(mesh):
    in_specs = (
        P("ep", None), P(), P(None, "tp"), P(None, "tp"), P(None, "tp"), P(None, "tp"), P("tp", None),
        P(("ep", "tp"), None), P(), P(("ep", "tp"), None), P(("ep", "tp"), None), P(("ep", "tp"), None),
        P("ep", None, "tp"), P("ep", None, "tp"), P("ep", "tp", None),
    )
    out_specs = (P(("ep", "tp"), None), P(("ep", "tp"), None))
    return jax.shard_map(
        on_device, mesh=mesh, in_specs=in_specs, out_specs=out_specs, check_vma=False
    )
```

```python
import jax
import jax.numpy as jnp
from jax import lax
from jax.experimental import pallas as pl
from jax.experimental.pallas import tpu as pltpu
from jax.sharding import PartitionSpec as P

MESH = pl.DeviceIdType.MESH
EPSILON = 1e-06
BF16 = jnp.bfloat16
F32 = jnp.float32
D = 2048
WIDE = D + 128
TOK = 160
HALF = 80
PER = 20
PAD = 32
GROUPS = 8
MEMBERS = 8
NX = 4
NY = 4
LOC = 256
CW = 512
SIZES = (512, 512, 512, 256, 256)
CHUNKS = len(SIZES)
STARTS = tuple(sum(SIZES[:k]) for k in range(CHUNKS))
COPIES = 160


def chunk(k):
    return pl.ds(STARTS[k], SIZES[k])


def dot(a, b):
    return jnp.dot(a, b, preferred_element_type=F32)


def iota(shape, dim):
    return lax.broadcasted_iota(jnp.int32, shape, dim)


def scaled(wide, gain):
    mean = jnp.mean(wide * wide, axis=-1, keepdims=True)
    return (wide * lax.rsqrt(mean + EPSILON) * gain).astype(BF16)


def kernel(
    mixer_input, mixer_gain, value_weight, inner_gate, outer_gate, taps, mixer_proj,
    expert_input, expert_gain, routes, group_logits, pair_logits, gate_weight, up_weight, down_weight,
    mixer_output, expert_output,
    m_in, w_v, w_i, w_o, w_p, e_in, w_g, w_u, w_d,
    rows, z_out, z_in, tokens, hidden, mixed, outer, m_rows, m_parts, from_prev, from_next,
    m_a, m_b, m_p, m_n,
    parts, pair, r_a, r_b, r_p, r_n, zr_out, zr_in, spread, unsort,
    send_sems, recv_sems, local_sems,
):
    ep = lax.axis_index("ep")
    y = lax.axis_index("tp")
    core = lax.rem(ep, 2)
    x = lax.rem(ep // 2, NX)
    z = ep // MEMBERS
    n_ep = GROUPS * MEMBERS

    def at(zz, xx, cc):
        return zz * MEMBERS + xx * 2 + cc

    y_next = (ep, lax.rem(y + 1, NY))
    y_prev = (ep, lax.rem(y + NY - 1, NY))
    x_next = (at(z, lax.rem(x + 1, NX), core), y)
    x_prev = (at(z, lax.rem(x + NX - 1, NX), core), y)
    twin = (at(z, x, 1 - core), y)
    s_next = (lax.rem(ep + 1, n_ep), y)
    s_prev = (lax.rem(ep + n_ep - 1, n_ep), y)
    z_plus = [(at(lax.rem(z + d, GROUPS), x, core), y) for d in range(GROUPS)]
    z_minus = [(at(lax.rem(z + GROUPS - d, GROUPS), x, core), y) for d in range(GROUPS)]

    locals_ = []

    def load(src, dst):
        copy = pltpu.make_async_copy(src, dst, local_sems.at[len(locals_)])
        locals_.append(copy)
        copy.start()
        return copy

    copies = []

    def send(src, dst, device):
        k = len(copies)
        copy = pltpu.make_async_remote_copy(
            src_ref=src, dst_ref=dst, send_sem=send_sems.at[k], recv_sem=recv_sems.at[k],
            device_id=device, device_id_type=MESH,
        )
        copies.append(copy)
        copy.start()
        return copy

    l_ein = load(expert_input, e_in)
    l_min = load(mixer_input, m_in)
    l_v = load(value_weight, w_v)
    l_i = load(inner_gate, w_i)
    l_o = load(outer_gate, w_o)
    l_p = load(mixer_proj, w_p)
    l_g = load(gate_weight.at[0], w_g.at[0])
    l_u = load(up_weight.at[0], w_u.at[0])
    l_d = load(down_weight.at[0], w_d.at[pl.ds(0, LOC)])

    barrier = pltpu.get_barrier_semaphore()
    partners = [y_next, y_prev, x_next, x_prev, twin, s_next, s_prev] + z_plus[1:]
    for device in partners:
        pl.semaphore_signal(barrier, inc=1, device_id=device, device_id_type=MESH)
    pl.semaphore_wait(barrier, len(partners))

    g_next = send(gate_weight.at[0], w_g.at[1], y_next)
    g_prev = send(gate_weight.at[0], w_g.at[3], y_prev)
    u_next = send(up_weight.at[0], w_u.at[1], y_next)
    u_prev = send(up_weight.at[0], w_u.at[3], y_prev)

    d_next = [None] * CHUNKS
    d_prev = [None] * CHUNKS

    def down_send(k):
        src = down_weight.at[0, :, chunk(k)]
        d_next[k] = send(src, w_d.at[pl.ds(LOC, LOC), chunk(k)], y_next)
        d_prev[k] = send(src, w_d.at[pl.ds(3 * LOC, LOC), chunk(k)], y_prev)

    down_send(0)

    fd_next = [None] * CHUNKS
    fd_prev = [None] * CHUNKS

    def down_forward(k):
        d_next[k].wait_recv()
        d_prev[k].wait_recv()
        half = SIZES[k] // 2
        left, right = pl.ds(STARTS[k], half), pl.ds(STARTS[k] + half, half)
        fd_next[k] = send(w_d.at[pl.ds(LOC, LOC), left], w_d.at[pl.ds(2 * LOC, LOC), left], y_next)
        fd_prev[k] = send(w_d.at[pl.ds(3 * LOC, LOC), right], w_d.at[pl.ds(2 * LOC, LOC), right], y_prev)

    l_ein.wait()
    e_gain = expert_gain[...]

    def norm_expert(i, _):
        at_ = pl.ds(pl.multiple_of(i * 32, 32), 32)
        rows[at_, pl.ds(0, D)] = scaled(e_in[at_, :].astype(F32), e_gain)
        return 0

    lax.fori_loop(0, TOK // 32, norm_expert, 0)
    first = routes[0:1, :]
    second = routes[1:2, :]
    group = lax.shift_right_logical(first, 3)
    logits = group_logits[...]
    picked = jnp.sum(jnp.where(iota((GROUPS, TOK), 0) == group, logits, 0.0), axis=0, keepdims=True)
    g_weight = 1.0 / jnp.sum(jnp.exp(logits - picked), axis=0, keepdims=True)
    p0 = pair_logits[0:1, :]
    p1 = pair_logits[1:2, :]
    weight0 = g_weight / (1.0 + jnp.exp(p1 - p0))
    weight1 = g_weight / (1.0 + jnp.exp(p0 - p1))
    line = iota((128, TOK), 0)
    member = lax.bitwise_and(line, 7)
    wide_w = jnp.where(member == lax.bitwise_and(first, 7), weight0, 0.0) + jnp.where(
        member == lax.bitwise_and(second, 7), weight1, 0.0
    )
    high = wide_w.astype(BF16).astype(F32)
    extra = jnp.where(line < 8, high, jnp.where(line < 16, wide_w - high, 0.0)).astype(BF16)

    rel_row = lax.bitwise_and(group + (GROUPS - z), 7).astype(F32)
    square = (TOK, TOK)
    sub, lan = iota(square, 0), iota(square, 1)
    rel_col = jnp.sum(jnp.where(sub == lan, rel_row, 0.0), axis=1, keepdims=True)
    earlier = (rel_col == rel_row) & (sub < lan)
    slot_row = rel_row * PAD + jnp.sum(jnp.where(earlier, 1.0, 0.0), axis=0, keepdims=True)
    slot_col = jnp.sum(jnp.where(sub == lan, slot_row, 0.0), axis=1, keepdims=True).astype(jnp.int32)
    slot_row = slot_row.astype(jnp.int32)
    sort = (iota((GROUPS * PAD, TOK), 0) == slot_row).astype(F32).astype(BF16)
    for q in range(4):
        cols = pl.ds(q * CW, CW)
        z_out[:, cols] = dot(sort, rows[:, cols]).astype(BF16)
    z_out[:, pl.ds(D, 128)] = lax.dot_general(
        sort, extra, (((1,), (1,)), ((), ())), preferred_element_type=F32
    ).astype(BF16)
    z_sent = [
        send(z_out.at[pl.ds(d * PAD, PAD)], z_in.at[pl.ds(d * PAD, PAD)], z_plus[d])
        for d in range(1, GROUPS)
    ]
    z_in[pl.ds(0, PAD), :] = z_out[pl.ds(0, PAD), :]
    unsort[...] = (iota((TOK, GROUPS * PAD), 1) == slot_col).astype(F32).astype(BF16)

    m_gain = mixer_gain[...]
    for copy in (l_min, l_v, l_i, l_o):
        copy.wait()

    def norm_mixer(i, _):
        at_ = pl.ds(pl.multiple_of(i * 32, 32), 32)
        m_in[at_, :] = scaled(m_in[at_, :].astype(F32), m_gain)
        return 0

    lax.fori_loop(0, NY * TOK // 32, norm_mixer, 0)

    def gates(i, _):
        at_ = pl.ds(pl.multiple_of(i * TOK, TOK), TOK)
        block = m_in[at_, :]
        value = dot(block, w_v[...])
        inner = dot(block, w_i[...])
        mixed[pl.ds(pl.multiple_of(i * TOK + 8, 8), TOK), :] = (inner * value).astype(BF16).astype(F32)
        outer[at_, :] = dot(block, w_o[...])
        return 0

    lax.fori_loop(0, NY, gates, 0)
    h_next = send(mixed.at[pl.ds(NY * TOK, 8)], from_prev, s_next)
    h_prev = send(mixed.at[pl.ds(8, 8)], from_next, s_prev)
    l_p.wait()
    h_next.wait_recv()
    h_prev.wait_recv()
    mixed[pl.ds(7, 1), :] = jnp.where(ep == 0, 0.0, from_prev[pl.ds(7, 1), :])
    mixed[pl.ds(NY * TOK + 8, 1), :] = jnp.where(ep == n_ep - 1, 0.0, from_next[pl.ds(0, 1), :])
    t0, t1, t2 = taps[0:1, :], taps[1:2, :], taps[2:3, :]
    for i in range(NY):
        at_ = i * TOK
        conv = (
            t0 * mixed[pl.ds(at_ + 7, TOK), :]
            + t1 * mixed[pl.ds(at_ + 8, TOK), :]
            + t2 * mixed[pl.ds(at_ + 9, TOK), :]
        )
        m_rows[pl.ds(at_, TOK), :] = (outer[pl.ds(at_, TOK), :] * conv).astype(BF16)

    def project(i, _):
        r = i // 4
        cols = pl.ds(pl.multiple_of(lax.rem(i, 4) * CW, CW), CW)
        begin = pl.multiple_of(lax.rem(y + r, NY) * TOK, TOK)
        block = m_rows[pl.ds(begin, TOK), :]
        m_parts[pl.ds(pl.multiple_of(r * TOK, TOK), TOK), cols] = dot(block, w_p[:, cols]).astype(BF16)
        return 0

    lax.fori_loop(0, NY * 4, project, 0)

    g_next.wait_recv()
    f_g = send(w_g.at[1], w_g.at[2], y_next)

    for copy in z_sent:
        copy.wait_recv()
    p_sub = iota((TOK, GROUPS * PAD), 0)
    shift = jnp.zeros((TOK, GROUPS * PAD), jnp.int32)
    for d in range(1, GROUPS):
        shift = shift + jnp.where(p_sub >= d * PER, PAD - PER, 0)
    compact = (iota((TOK, GROUPS * PAD), 1) == p_sub + shift).astype(F32).astype(BF16)
    q_lan = iota((GROUPS * PAD, TOK), 1)
    shift = jnp.zeros((GROUPS * PAD, TOK), jnp.int32)
    for d in range(1, GROUPS):
        shift = shift + jnp.where(q_lan >= d * PER, PAD - PER, 0)
    spread[...] = (iota((GROUPS * PAD, TOK), 0) == q_lan + shift).astype(F32).astype(BF16)
    for q in range(4):
        cols = pl.ds(q * CW, CW)
        tokens[pl.ds(0, TOK), cols] = dot(compact, z_in[:, cols]).astype(BF16)
    tokens[pl.ds(0, TOK), pl.ds(D, 128)] = dot(compact, z_in[:, pl.ds(D, 128)]).astype(BF16)

    def block(b, h=None):
        if h is None:
            return tokens.at[pl.ds(b * TOK, TOK)]
        return tokens.at[pl.ds(b * TOK + h * HALF, HALF)]

    a_next = [None, None]
    a_prev = [None, None]
    a_next[0] = send(block(0, 0), block(1, 0), x_next)
    a_prev[1] = send(block(0, 1), block(3, 1), x_prev)
    a_next[1] = send(block(0, 1), block(1, 1), x_next)
    a_prev[0] = send(block(0, 0), block(3, 0), x_prev)
    c_own = send(block(0), block(4), twin)
    a_next[0].wait_recv()
    f_next = send(block(1, 0), block(2, 0), x_next)
    a_prev[1].wait_recv()
    f_prev = send(block(3, 1), block(2, 1), x_prev)
    u_prev.wait_recv()
    f_u = send(w_u.at[3], w_u.at[2], y_prev)
    down_send(1)
    down_forward(0)
    down_send(2)
    a_next[1].wait_recv()
    c_1 = send(block(1), block(5), twin)
    a_prev[0].wait_recv()
    c_3 = send(block(3), block(7), twin)

    f_next.wait_recv()
    f_prev.wait_recv()
    c_2 = send(block(2), block(6), twin)
    for copy in (c_own, c_1, c_3, c_2):
        copy.wait_recv()

    TILE = 320
    TILES = MEMBERS * TOK // TILE

    def ffn(j):
        def body(i, _):
            at_ = pl.ds(pl.multiple_of(i * TILE, TILE), TILE)
            block_ = tokens[at_, pl.ds(0, D)]
            a = dot(block_, w_g[j])
            b = dot(block_, w_u[j])
            hidden[at_, pl.ds(j * LOC, LOC)] = (a / (1.0 + jnp.exp(-a)) * b).astype(BF16)
            return 0

        lax.fori_loop(0, TILES, body, 0)

    l_g.wait()
    l_u.wait()
    ffn(0)
    u_next.wait_recv()
    ffn(1)
    g_prev.wait_recv()
    ffn(3)
    f_g.wait_recv()
    f_u.wait_recv()
    ffn(2)
    l_d.wait()

    own = x * 2 + core
    e_sent = [None] * CHUNKS
    ra = [None] * CHUNKS
    rb = [None] * CHUNKS
    n_a = [None] * CHUNKS
    n_b = [None] * CHUNKS
    p_a = [None] * CHUNKS
    p_b = [None] * CHUNKS
    z_back = [None] * CHUNKS

    def results(k):
        fd_next[k].wait_recv()
        fd_prev[k].wait_recv()

        def body(i, _):
            at_ = pl.ds(pl.multiple_of(i * TILE, TILE), TILE)
            both = tokens[at_, pl.ds(D, 128)].astype(F32)
            lane_ = iota((TILE, 128), 1)
            mine = (lane_ == own) | (lane_ == own + 8)
            weight = jnp.sum(jnp.where(mine, both, 0.0), axis=1, keepdims=True)
            parts[at_, chunk(k)] = (dot(hidden[at_, :], w_d[:, chunk(k)]) * weight).astype(BF16)
            return 0

        lax.fori_loop(0, TILES, body, 0)
        e_sent[k] = send(parts.at[pl.ds(NX * TOK, NX * TOK), chunk(k)], pair.at[:, chunk(k)], twin)

    def add_into(ref, k, begin, count, other):
        at_ = pl.ds(begin, count)
        ref[at_, chunk(k)] = (ref[at_, chunk(k)].astype(F32) + other.astype(F32)).astype(BF16)

    def merge(k):
        e_sent[k].wait_recv()
        for rx in (2, 3, 1, 0):
            add_into(parts, k, rx * TOK, TOK, pair[pl.ds(rx * TOK, TOK), chunk(k)])
        rb[k] = send(parts.at[pl.ds(2 * TOK + HALF, HALF), chunk(k)], r_b.at[:, chunk(k)], x_next)
        ra[k] = send(parts.at[pl.ds(2 * TOK, HALF), chunk(k)], r_a.at[:, chunk(k)], x_prev)
        n_a[k] = send(parts.at[pl.ds(3 * TOK, HALF), chunk(k)], r_p.at[pl.ds(0, HALF), chunk(k)], x_next)
        p_b[k] = send(parts.at[pl.ds(TOK + HALF, HALF), chunk(k)], r_n.at[pl.ds(HALF, HALF), chunk(k)], x_prev)

    def relay(k):
        rb[k].wait_recv()
        add_into(parts, k, 3 * TOK + HALF, HALF, r_b[:, chunk(k)])
        n_b[k] = send(parts.at[pl.ds(3 * TOK + HALF, HALF), chunk(k)], r_p.at[pl.ds(HALF, HALF), chunk(k)], x_next)
        ra[k].wait_recv()
        add_into(parts, k, TOK, HALF, r_a[:, chunk(k)])
        p_a[k] = send(parts.at[pl.ds(TOK, HALF), chunk(k)], r_n.at[pl.ds(0, HALF), chunk(k)], x_prev)

    def arrive(k):
        for copy in (n_a[k], p_b[k], n_b[k], p_a[k]):
            copy.wait_recv()
        total = (
            parts[pl.ds(0, TOK), chunk(k)].astype(F32) + r_p[:, chunk(k)].astype(F32) + r_n[:, chunk(k)].astype(F32)
        ).astype(BF16)
        zr_out[:, chunk(k)] = dot(spread[...], total).astype(BF16)
        z_back[k] = [
            send(zr_out.at[pl.ds(d * PAD, PAD), chunk(k)], zr_in.at[pl.ds(d * PAD, PAD), chunk(k)], z_minus[d])
            for d in range(1, GROUPS)
        ]
        zr_in[pl.ds(0, PAD), chunk(k)] = zr_out[pl.ds(0, PAD), chunk(k)]

    def finish(k):
        for copy in z_back[k]:
            copy.wait_recv()
        expert_output[:, chunk(k)] = dot(unsort[...], zr_in[:, chunk(k)]).astype(BF16)

    def m_add(begin, other):
        def body(i, _):
            cols = pl.ds(pl.multiple_of(i * CW, CW), CW)
            at_ = pl.ds(begin, HALF)
            m_parts[at_, cols] = (m_parts[at_, cols].astype(F32) + other[:, cols].astype(F32)).astype(BF16)
            return 0

        lax.fori_loop(0, 4, body, 0)

    down_forward(1)
    down_send(3)
    results(0)
    merge(0)
    down_forward(2)
    down_send(4)
    results(1)
    relay(0)
    down_forward(3)
    merge(1)
    results(2)
    down_forward(4)
    mb = send(m_parts.at[pl.ds(2 * TOK + HALF, HALF)], m_b, y_next)
    ma = send(m_parts.at[pl.ds(2 * TOK, HALF)], m_a, y_prev)
    mn_a = send(m_parts.at[pl.ds(TOK, HALF)], m_p.at[pl.ds(0, HALF)], y_next)
    mp_b = send(m_parts.at[pl.ds(3 * TOK + HALF, HALF)], m_n.at[pl.ds(HALF, HALF)], y_prev)
    arrive(0)
    relay(1)
    merge(2)
    results(3)
    results(4)
    merge(3)
    merge(4)
    arrive(1)
    relay(2)
    relay(3)
    relay(4)
    finish(0)
    mb.wait_recv()
    m_add(TOK + HALF, m_b)
    mn_b = send(m_parts.at[pl.ds(TOK + HALF, HALF)], m_p.at[pl.ds(HALF, HALF)], y_next)
    ma.wait_recv()
    m_add(3 * TOK, m_a)
    mp_a = send(m_parts.at[pl.ds(3 * TOK, HALF)], m_n.at[pl.ds(0, HALF)], y_prev)
    arrive(2)
    arrive(3)
    arrive(4)
    for k in range(1, CHUNKS):
        finish(k)
    for copy in (mn_a, mp_b, mn_b, mp_a):
        copy.wait_recv()

    def m_final(i, _):
        cols = pl.ds(pl.multiple_of(i * CW, CW), CW)
        mixer_output[:, cols] = (
            m_parts[pl.ds(0, TOK), cols].astype(F32) + m_p[:, cols].astype(F32) + m_n[:, cols].astype(F32)
        ).astype(BF16)
        return 0

    lax.fori_loop(0, 4, m_final, 0)
    for copy in copies:
        copy.wait_send()


def deliver(a, b, a_out, b_out, held, sems):
    loads = [pltpu.make_async_copy(r, held.at[k], sems.at[k]) for k, r in enumerate((a, b))]
    stores = [pltpu.make_async_copy(held.at[k], r, sems.at[k + 2]) for k, r in enumerate((a_out, b_out))]
    for copy in loads:
        copy.start()
    for copy, store in zip(loads, stores):
        copy.wait()
        store.start()
    for store in stores:
        store.wait()


def on_device(*args):
    args = list(args)
    args[1] = args[1].reshape(1, D)
    args[8] = args[8].reshape(1, D)
    for k in (9, 10, 11):
        args[k] = args[k].T
    any_ = pl.BlockSpec(memory_space=pl.ANY)
    vmem = pl.BlockSpec(memory_space=pltpu.VMEM)
    big = (0, 2, 3, 4, 6, 7, 12, 13, 14)
    out = jax.ShapeDtypeStruct((TOK, D), BF16)
    rows = MEMBERS * TOK
    scratch = [
        pltpu.VMEM((NY * TOK, D), BF16),
        pltpu.VMEM((D, LOC), BF16),
        pltpu.VMEM((D, LOC), BF16),
        pltpu.VMEM((D, LOC), BF16),
        pltpu.VMEM((LOC, D), BF16),
        pltpu.VMEM((TOK, D), BF16),
        pltpu.VMEM((NY, D, LOC), BF16),
        pltpu.VMEM((NY, D, LOC), BF16),
        pltpu.VMEM((NY * LOC, D), BF16),
        pltpu.VMEM((TOK, D), BF16),
        pltpu.VMEM((GROUPS * PAD, WIDE), BF16),
        pltpu.VMEM((GROUPS * PAD, WIDE), BF16),
        pltpu.VMEM((rows, WIDE), BF16),
        pltpu.VMEM((rows, NY * LOC), BF16),
        pltpu.VMEM((NY * TOK + 16, LOC), F32),
        pltpu.VMEM((NY * TOK, LOC), F32),
        pltpu.VMEM((NY * TOK, LOC), BF16),
        pltpu.VMEM((NY * TOK, D), BF16),
        pltpu.VMEM((8, LOC), F32),
        pltpu.VMEM((8, LOC), F32),
        pltpu.VMEM((HALF, D), BF16),
        pltpu.VMEM((HALF, D), BF16),
        pltpu.VMEM((TOK, D), BF16),
        pltpu.VMEM((TOK, D), BF16),
        pltpu.VMEM((rows, D), BF16),
        pltpu.VMEM((NX * TOK, D), BF16),
        pltpu.VMEM((HALF, D), BF16),
        pltpu.VMEM((HALF, D), BF16),
        pltpu.VMEM((TOK, D), BF16),
        pltpu.VMEM((TOK, D), BF16),
        pltpu.VMEM((GROUPS * PAD, D), BF16),
        pltpu.VMEM((GROUPS * PAD, D), BF16),
        pltpu.VMEM((GROUPS * PAD, TOK), BF16),
        pltpu.VMEM((TOK, GROUPS * PAD), BF16),
        pltpu.SemaphoreType.DMA((COPIES,)),
        pltpu.SemaphoreType.DMA((COPIES,)),
        pltpu.SemaphoreType.DMA((16,)),
    ]
    results = pl.pallas_call(
        kernel,
        out_shape=(out, out),
        in_specs=[any_ if k in big else vmem for k in range(15)],
        out_specs=(vmem, vmem),
        scratch_shapes=scratch,
        compiler_params=pltpu.CompilerParams(
            collective_id=0, has_side_effects=True, vmem_limit_bytes=67043328
        ),
        name="mixer_and_experts",
    )(*args)
    return pl.pallas_call(
        deliver,
        out_shape=(out, out),
        in_specs=[any_, any_],
        out_specs=(any_, any_),
        scratch_shapes=[pltpu.VMEM((2, TOK, D), BF16), pltpu.SemaphoreType.DMA((4,))],
        name="deliver",
    )(*results)


def solution(mesh):
    in_specs = (
        P("ep", None), P(), P(None, "tp"), P(None, "tp"), P(None, "tp"), P(None, "tp"), P("tp", None),
        P(("ep", "tp"), None), P(), P(("ep", "tp"), None), P(("ep", "tp"), None), P(("ep", "tp"), None),
        P("ep", None, "tp"), P("ep", None, "tp"), P("ep", "tp", None),
    )
    out_specs = (P(("ep", "tp"), None), P(("ep", "tp"), None))
    return jax.shard_map(
        on_device, mesh=mesh, in_specs=in_specs, out_specs=out_specs, check_vma=False
    )
```
